32 devices in a mesh: grp: 2 (over y), sp: 4 (over z), tp: 4 (over x, core).
Axes of the slice: x: 2, y: 2, z: 4, core: 2. Of those that a mesh axis runs over, the one named last changes fastest.
Arguments:
- residual: bfloat16 [2048, 2048], P(('grp', 'sp', 'tp')), parts along dimension 0, may hold values from -6 to 6
- query_nope: bfloat16 [2048, 1024], P(('grp', 'sp'), 'tp'), parts along dimension 0, may hold values from -6 to 6
- query_rope: bfloat16 [2048, 512], P(('grp', 'sp'), 'tp'), parts along dimension 0, may hold values from -240 to 240
- kv_latent: bfloat16 [2048, 256], P(('grp', 'sp')), parts along dimension 0, may hold values from -6 to 6
- rope_key: bfloat16 [2048, 64], P(('grp', 'sp')), parts along dimension 0, may hold values from -6 to 6
- latent_gain: float32 [256], replicated, may hold values from 0.1 to 1.9
- w_key: bfloat16 [256, 1024], P(None, 'tp'), may hold values from -0.375 to 0.375
- w_value: bfloat16 [256, 1024], P(None, 'tp'), may hold values from -0.375 to 0.375
- w_out: bfloat16 [1024, 2048], P('tp'), may hold values from -0.1875 to 0.1875
- post_gain: float32 [2048], replicated, may hold values from 0.1 to 1.9
- routes: int32 [2048, 2], P(('grp', 'sp', 'tp')), parts along dimension 0, may hold values from 0 to 3, all different within a row; in each aligned block of 64 rows (0 to 63, 64 to 127, ...) at most 48 rows name the same one
- route_weight: float32 [2048, 2], P(('grp', 'sp', 'tp')), parts along dimension 0, may hold values from 0.25 to 1
- moe_gain: float32 [2048], replicated, may hold values from 0.1 to 1.9
- w_gate: bfloat16 [4, 2048, 3584], P('sp', None, 'tp'), may hold values from -0.125 to 0.125
- w_up: bfloat16 [4, 2048, 3584], P('sp', None, 'tp'), may hold values from -0.125 to 0.125
- w_down: bfloat16 [4, 3584, 2048], P('sp', 'tp'), may hold values from -0.09375 to 0.09375
Outputs:
- mixed: bfloat16 [2048, 2048], P(('grp', 'sp', 'tp')), parts along dimension 0
The draws below stay inside these ranges and needn't reach their ends.
There are 2 independent parts, one for each index of `grp`. The reference program is written for one: setup_inputs(seed, part) draws one part's arguments, and reference() takes and returns one part's arrays. A program takes and returns all parts, laid end to end along the dimension named above; an argument that names none is the same for every part. Nothing has to cross between parts.
Inputs may be any that keep to these rules, and one draw needn't show every extreme that they name: `routes`: each row names two different experts. Among the 64 rows of one device no expert is named more than 48 times, and some device names some expert exactly 48 times.
All inputs are finite; a program needn't handle non-finite values.
Results may differ from the reference program's by a relative error of at most 0.014.
Values may be sent and summed in bfloat16 or wider, within the bound.
A program may use at most 128 MiB of HBM per device.

```python
import math
import jax
import jax.numpy as jnp
import numpy as np
from jax import lax

D = 2048
HEADS = 8
NOPE = 128
ROPE = 64
VDIM = 128
KV_RANK = 256
FF = 3584
SEQ = 1024
TOK_DEV = 64
EXPERTS = 4
CAP = 48
N_SP = 4
N_TP = 4


def draw_query_rope(key, part):
    shape = (SEQ, HEADS * ROPE)
    values = jax.random.normal(jax.random.fold_in(key, 11), shape, jnp.float32)
    return jnp.clip(values, -240.0, 240.0).astype(jnp.bfloat16)


def block_scale(own_key, dims, split, least, high):
    gain = 1.0
    for dim, parts in split:
        steps = jax.random.uniform(jax.random.fold_in(jax.random.fold_in(own_key, 6), dim), (parts,), jnp.float32, least / len(split), high / len(split))
        gain = gain * jnp.repeat(jnp.exp(steps), dims[dim] // parts).reshape((-1,) + (1,) * (len(dims) - 1 - dim))
    return gain


def assign_block(key, own, number, rows, number_of, top, reach, lean):
    order = jax.random.permutation(key, number_of)
    heavy_load, ordinary = load_shares(number_of, rows * top, reach, lean, True), load_shares(number_of, rows * top, reach, lean, False)
    places = jnp.arange(number_of)

    def named(lengths, offset_by):
        used = int((lengths > 0).sum())
        fixed = max(1, used // 4)
        moved = fixed + (places - fixed + offset_by * (used - fixed)) % max(1, number_of - fixed)
        return jnp.zeros((number_of,), jnp.int32).at[order[jnp.where(places < fixed, places, moved)]].set(jnp.asarray(lengths, jnp.int32))

    lengths = jnp.where(number % 4 == 0, named(heavy_load, number // 4), named(ordinary, number - number // 4 - 1))
    mixed = jax.random.permutation(jax.random.fold_in(own, 3), number_of)
    giver, receiver = mixed[0:number_of // 2 * 2:2], mixed[1:number_of // 2 * 2:2]
    room = jnp.minimum(lengths[giver] - 1, reach - lengths[receiver]) // 2
    room = jnp.where((giver == order[0]) | (receiver == order[0]) | (lengths[receiver] == 0), 0, jnp.maximum(room, 0))
    moved = jax.random.randint(jax.random.fold_in(own, 4), (number_of // 2,), 0, 1 << 20) % (room + 1)
    lengths = lengths.at[giver].add(-moved).at[receiver].add(moved)
    items = jnp.searchsorted(jnp.cumsum(lengths), jnp.arange(rows * top), side="right").astype(jnp.int32)
    table = items.reshape(top, rows).T
    table = table[jax.random.permutation(jax.random.fold_in(own, 1), rows)]
    offset_by = jax.random.randint(jax.random.fold_in(own, 2), (rows, 1), 0, top)
    return jnp.take_along_axis(table, (jnp.arange(top)[None, :] + offset_by) % top, axis=1)


def load_shares(count, total, bound, lean, full):
    loads = [(1 << 20) // math.isqrt(grade ** lean) + 1 for grade in range(1, count + 1)]
    largest = bound if full else min(bound, max(-(-total // count), total * loads[0] // sum(loads)))
    least = 1 if total - largest >= count - 1 else 0
    given, rest = [largest] + [least] * (count - 1), total - largest - least * (count - 1)
    while rest > 0:
        movable = [i for i in range(1, count) if given[i] < largest] or [i for i in range(1, count) if given[i] < bound]
        pool, budget = sum([loads[i] for i in movable]), rest
        for i in movable:
            addition = min(bound - given[i], max(1, budget * loads[i] // pool), rest)
            given[i] = given[i] + addition
            rest = rest - addition
    return np.array(given)


def normal_values(stream_key, dims, width, limit, cuts=(), kind=jnp.bfloat16):
    factor_of = block_scale(stream_key, dims, cuts, -0.22, 0.18) if cuts else 1.0
    drawn = jax.random.normal(stream_key, dims, jnp.float32) * width * factor_of
    return jnp.minimum(jnp.maximum(drawn, -limit), limit).astype(kind)


def setup_inputs(seed: int = 0, part: int = 0) -> dict:
    splits = jax.random.split(jax.random.key(seed), 17)
    part_splits = jax.random.split(jax.random.fold_in(splits[16], part), 17)
    residual = normal_values(part_splits[0], (SEQ, D), 1.0, 6.0, ((0, 16),))
    query_nope = normal_values(part_splits[1], (SEQ, HEADS * NOPE), 1.0, 6.0, ((0, 4), (1, 4)))
    query_rope = draw_query_rope(jax.random.fold_in(jax.random.fold_in(splits[16], part), 71), part)
    kv_latent = normal_values(part_splits[3], (SEQ, KV_RANK), 1.0, 6.0, ((0, 4),))
    rope_key = normal_values(part_splits[4], (SEQ, ROPE), 1.0, 6.0, ((0, 4),))
    latent_gain = jnp.clip(1.0 + 0.18 * jax.random.normal(splits[5], (KV_RANK,), jnp.float32), 0.1, 1.9)
    w_key = normal_values(splits[6], (KV_RANK, HEADS * NOPE), KV_RANK ** -0.5, 0.375, ((1, 4),))
    w_value = normal_values(splits[7], (KV_RANK, HEADS * VDIM), KV_RANK ** -0.5, 0.375, ((1, 4),))
    w_out = normal_values(splits[8], (HEADS * VDIM, D), (HEADS * VDIM) ** -0.5, 0.1875, ((0, 4),))
    post_gain = jnp.clip(1.0 + 0.18 * jax.random.normal(splits[9], (D,), jnp.float32), 0.1, 1.9)
    routes_keys = jax.random.split(jax.random.fold_in(part_splits[10], 1), SEQ // TOK_DEV)
    routes_turns = jax.random.permutation(jax.random.fold_in(part_splits[10], 3), SEQ // TOK_DEV)
    routes = jax.vmap(lambda own, number: assign_block(jax.random.fold_in(part_splits[10], 2), own, number, TOK_DEV, EXPERTS, 2, CAP, 2))(routes_keys, routes_turns).reshape((SEQ, 2))
    route_weight = jnp.clip(0.25 + 0.75 * jax.random.uniform(part_splits[11], (SEQ, 2), jnp.float32) ** block_scale(part_splits[11], (SEQ, 2), ((0, 16),), -0.2, 0.2), 0.25, 1.0)
    moe_gain = jnp.clip(1.0 + 0.18 * jax.random.normal(splits[12], (D,), jnp.float32), 0.1, 1.9)
    w_gate = normal_values(splits[13], (EXPERTS, D, FF), D ** -0.5, 0.125, ((0, 4), (2, 4)))
    w_up = normal_values(splits[14], (EXPERTS, D, FF), D ** -0.5, 0.125, ((0, 4), (2, 4)))
    w_down = normal_values(splits[15], (EXPERTS, FF, D), FF ** -0.5, 0.09375, ((0, 4), (1, 4)))
    return dict(residual=residual, query_nope=query_nope, query_rope=query_rope, kv_latent=kv_latent, rope_key=rope_key, latent_gain=latent_gain, w_key=w_key, w_value=w_value, w_out=w_out, post_gain=post_gain, routes=routes, route_weight=route_weight, moe_gain=moe_gain, w_gate=w_gate, w_up=w_up, w_down=w_down)


epsilon = 1e-06
rope_base = 10000.0

def rms_scale(inputs, gain_vector):
    mean_square = lax.optimization_barrier(jnp.mean(inputs * inputs, axis=-1, keepdims=True))
    return inputs * lax.rsqrt(mean_square + epsilon) * gain_vector.astype(jnp.float32)

def tables(positions, rot_width):
    frequency = 1.0 / rope_base ** (jnp.arange(0, rot_width, 2, dtype=jnp.float32) / rot_width)
    angles = positions.astype(jnp.float32)[:, None] * frequency[None, :]
    return (jnp.cos(angles), jnp.sin(angles))

def rotate(inputs, cosine_table, sine_table):
    half_width = inputs.shape[-1] // 2
    first_half = inputs[..., :half_width]
    second_half = inputs[..., half_width:]
    return jnp.concatenate([first_half * cosine_table - second_half * sine_table, second_half * cosine_table + first_half * sine_table], axis=-1)

def reference(residual, query_nope, query_rope, kv_latent, rope_key, latent_gain, w_key, w_value, w_out, post_gain, routes, route_weight, moe_gain, w_gate, w_up, w_down):
    seq_len = residual.shape[0]
    positions = jnp.arange(seq_len, dtype=jnp.int32)
    cosine_table, sine_table = tables(positions, ROPE)
    normed = rms_scale(kv_latent.astype(jnp.float32), latent_gain).astype(jnp.bfloat16)
    key_plain = jnp.dot(normed, w_key, preferred_element_type=jnp.float32).astype(jnp.bfloat16)
    value_plain = jnp.dot(normed, w_value, preferred_element_type=jnp.float32).astype(jnp.bfloat16)
    key_heads = key_plain.reshape(seq_len, HEADS, NOPE).astype(jnp.float32)
    value_heads = value_plain.reshape(seq_len, HEADS, VDIM).astype(jnp.float32)
    key_turned = rotate(rope_key.astype(jnp.float32), cosine_table, sine_table).astype(jnp.bfloat16).astype(jnp.float32)
    query_plain = query_nope.reshape(seq_len, HEADS, NOPE)
    query_turned = rotate(query_rope.reshape(seq_len, HEADS, ROPE).astype(jnp.float32), cosine_table[:, None, :], sine_table[:, None, :]).astype(jnp.bfloat16)
    score_scale = (NOPE + ROPE) ** (-0.5)
    block_len = math.gcd(seq_len, 512)

    def one_block(block_index):
        block_begin = block_index * block_len
        query_block = lax.dynamic_slice_in_dim(query_plain, block_begin, block_len, 0).astype(jnp.float32)
        turned_block = lax.dynamic_slice_in_dim(query_turned, block_begin, block_len, 0).astype(jnp.float32)
        scores = jnp.einsum('thd,shd->hts', query_block, key_heads)
        scores = (scores + jnp.einsum('thd,sd->hts', turned_block, key_turned)) * score_scale
        query_pos = block_begin + jnp.arange(block_len, dtype=jnp.int32)
        allowed = positions[None, :] <= query_pos[:, None]
        scores = jnp.where(allowed[None], scores, -jnp.inf)
        row_max = lax.optimization_barrier(jnp.max(scores, axis=-1, keepdims=True))
        expo = jnp.exp(scores - row_max)
        row_sum = lax.optimization_barrier(jnp.sum(expo, axis=-1))
        probs = lax.optimization_barrier(expo.astype(jnp.bfloat16)).astype(jnp.float32)
        weighted = jnp.einsum('hts,shd->htd', probs, value_heads) / row_sum[..., None]
        return weighted.transpose(1, 0, 2).reshape(block_len, HEADS * VDIM).astype(jnp.bfloat16)
    attended = lax.map(one_block, jnp.arange(seq_len // block_len, dtype=jnp.int32)).reshape(seq_len, HEADS * VDIM)
    group_rows = HEADS * VDIM // N_TP
    branch = jnp.zeros((seq_len, D), jnp.float32)
    for group_id in range(N_TP):
        partial_value = jnp.dot(attended[:, group_id * group_rows:(group_id + 1) * group_rows], w_out[group_id * group_rows:(group_id + 1) * group_rows], preferred_element_type=jnp.float32).astype(jnp.bfloat16)
        branch = branch + lax.optimization_barrier(partial_value).astype(jnp.float32)
    updated = (residual.astype(jnp.float32) + rms_scale(branch, post_gain)).astype(jnp.bfloat16)
    moe_in = rms_scale(updated.astype(jnp.float32), moe_gain).astype(jnp.bfloat16)
    flat_routes = routes.reshape(-1)
    flat_weight = route_weight.reshape(-1).astype(jnp.float32)
    token_ids = jnp.arange(flat_routes.shape[0], dtype=jnp.int32) // 2
    slot_bound = N_SP * N_TP * CAP
    group_width = FF // N_TP

    def one_expert(summed, inputs):
        gate_matrix, up_matrix, down_matrix, expert_id = inputs
        matches = flat_routes == expert_id
        found, = jnp.nonzero(matches, size=slot_bound, fill_value=0)
        filled = (jnp.arange(slot_bound, dtype=jnp.int32) < jnp.sum(matches.astype(jnp.int32))).astype(jnp.float32)
        picked = moe_in[token_ids[found]]
        gate_pre = jnp.dot(picked, gate_matrix, preferred_element_type=jnp.float32)
        up_proj = jnp.dot(picked, up_matrix, preferred_element_type=jnp.float32)
        activated = (jax.nn.silu(gate_pre) * up_proj).astype(jnp.bfloat16)
        grouped = activated.reshape(slot_bound, N_TP, group_width).transpose(1, 0, 2).astype(jnp.float32)
        down_groups = down_matrix.reshape(N_TP, group_width, D).astype(jnp.float32)
        partials = jnp.einsum('gra,gad->grd', grouped, down_groups).astype(jnp.bfloat16)
        partials = lax.optimization_barrier(partials)
        expert_out = lax.optimization_barrier(lax.optimization_barrier(jnp.sum(partials.astype(jnp.float32), axis=0)).astype(jnp.bfloat16))
        scaled = expert_out.astype(jnp.float32) * (flat_weight[found] * filled)[:, None]
        summed = summed.at[token_ids[found]].add(scaled)
        return (summed, None)
    summed, _ = lax.scan(one_expert, jnp.zeros((seq_len, D), jnp.float32), (w_gate, w_up, w_down, jnp.arange(EXPERTS, dtype=jnp.int32)))
    return (updated.astype(jnp.float32) + summed).astype(jnp.bfloat16)
```

```python
import functools

import jax
import jax.numpy as jnp
from jax import lax
from jax.experimental import pallas as pl
from jax.experimental.pallas import tpu as pltpu
from jax.sharding import PartitionSpec as P

MESH = pl.DeviceIdType.MESH

HEADS = 8
NOPE = 128
ROPE = 64
VDIM = 128


epsilon = 1e-06
rope_base = 10000.0


def rms_scale(inputs, gain_vector):
    mean_square = jnp.mean(inputs * inputs, axis=-1, keepdims=True)
    return inputs * lax.rsqrt(mean_square + epsilon) * gain_vector


def tables(positions, rot_width):
    frequency = 1.0 / rope_base ** (jnp.arange(0, rot_width, 2, dtype=jnp.float32) / rot_width)
    angles = positions.astype(jnp.float32)[:, None] * frequency[None, :]
    return (jnp.cos(angles), jnp.sin(angles))


def rotate(inputs, cosine_table, sine_table):
    half_width = inputs.shape[-1] // 2
    first_half = inputs[..., :half_width]
    second_half = inputs[..., half_width:]
    return jnp.concatenate(
        [
            first_half * cosine_table - second_half * sine_table,
            second_half * cosine_table + first_half * sine_table,
        ],
        axis=-1,
    )


def expand(latent_rows, rope_rows, latent_gain, w_key, w_value):
    normed = rms_scale(latent_rows.astype(jnp.float32), latent_gain).astype(jnp.bfloat16)
    key_plain = jnp.dot(normed, w_key, preferred_element_type=jnp.float32).astype(jnp.bfloat16)
    value_plain = jnp.dot(normed, w_value, preferred_element_type=jnp.float32).astype(jnp.bfloat16)
    key_positions = jnp.arange(latent_rows.shape[0], dtype=jnp.int32)
    cosine_table, sine_table = tables(key_positions, rope_rows.shape[1])
    key_turned = rotate(rope_rows.astype(jnp.float32), cosine_table, sine_table).astype(
        jnp.bfloat16
    )
    return (key_plain, value_plain, key_turned)


def push(source, target, send_sem, recv_sem, where):
    return pltpu.make_async_remote_copy(
        src_ref=source,
        dst_ref=target,
        send_sem=send_sem,
        recv_sem=recv_sem,
        device_id=where,
        device_id_type=MESH,
    )


def greet(places):
    barrier = pltpu.get_barrier_semaphore()
    for place in places:
        pl.semaphore_signal(barrier, inc=1, device_id=place, device_id_type=MESH)
    pl.semaphore_wait(barrier, len(places))


def tp_peers():
    me = lax.axis_index("tp")
    high, low = me // 2, me % 2
    return me, 2 * (1 - high) + low, 2 * high + (1 - low), 2 * (1 - high) + (1 - low)


def keys_kernel(n_sp, own_ref, all_ref, out_sem, in_sem, pass_sem, passed_sem):
    here = lax.axis_index("sp")
    me, _, pair, _ = tp_peers()
    low = me % 2
    greet([{"sp": lax.rem(here + k, n_sp)} for k in range(1, n_sp)] + [{"tp": pair}])

    def outward(k):
        there = lax.rem(here + k, n_sp)
        return push(
            own_ref.at[low], all_ref.at[here, low], out_sem.at[k], in_sem.at[here], {"sp": there}
        )

    def inward(k):
        there = lax.rem(here - k + n_sp, n_sp)
        return push(
            own_ref.at[low], all_ref.at[there, low], out_sem.at[k], in_sem.at[there], {"sp": there}
        )

    def relay(k, half):
        there = lax.rem(here - k + n_sp, n_sp)
        return push(
            all_ref.at[there, half],
            all_ref.at[there, half],
            pass_sem.at[k],
            passed_sem.at[there],
            {"tp": pair},
        )

    def begin(k, carry):
        @pl.when(here + k < n_sp)
        def _():
            outward(k).start()

        return carry

    lax.fori_loop(1, n_sp, begin, 0)
    all_ref[here] = own_ref[...]

    def clear(k, carry):
        @pl.when(here + k < n_sp)
        def _():
            all_ref[here + k] = jnp.zeros(own_ref.shape, own_ref.dtype)

        return carry

    lax.fori_loop(1, n_sp, clear, 0)

    def forward(k, carry):
        @pl.when(here >= k)
        def _():
            inward(k).wait_recv()
            relay(k, low).start()

        return carry

    lax.fori_loop(1, n_sp, forward, 0)

    def finish(k, carry):
        @pl.when(here >= k)
        def _():
            relay(k, 1 - low).wait_recv()
            relay(k, low).wait_send()

        @pl.when(here + k < n_sp)
        def _():
            outward(k).wait_send()

        return carry

    lax.fori_loop(1, n_sp, finish, 0)


def gather_keys(own_rows):
    n_sp = lax.axis_size("sp")
    rows, width = own_rows.shape
    sems = [pltpu.SemaphoreType.DMA((n_sp,))] * 4
    gathered = pl.pallas_call(
        functools.partial(keys_kernel, n_sp),
        out_shape=jax.ShapeDtypeStruct((n_sp, 2, rows // 2, width), own_rows.dtype),
        in_specs=[pl.BlockSpec(memory_space=pltpu.VMEM)],
        out_specs=pl.BlockSpec(memory_space=pltpu.VMEM),
        scratch_shapes=sems,
        compiler_params=pltpu.CompilerParams(collective_id=0, has_side_effects=True),
        name="gather_keys",
    )(own_rows.reshape(2, rows // 2, width))
    return gathered.reshape(n_sp * rows, width)


def branch_kernel(
    pieces, part_ref, sum_ref, far_in, own_in, mixed_out, mixed_in, a_s, a_r, b_s, b_r, c_s, c_r
):
    me, across, pair, far = tp_peers()
    greet([{"tp": pair}, {"tp": across}])

    def far_copy(j):
        return push(part_ref.at[far, j], far_in.at[j], a_s.at[j], a_r.at[j], {"tp": pair})

    def own_copy():
        return push(part_ref.at[pair], own_in, b_s, b_r, {"tp": pair})

    def across_copy(j):
        return push(mixed_out.at[j], mixed_in.at[j], c_s.at[j], c_r.at[j], {"tp": across})

    for j in range(pieces):
        far_copy(j).start()
    own_copy().start()
    for j in range(pieces):
        far_copy(j).wait_recv()
        total = part_ref[across, j].astype(jnp.float32) + far_in[j].astype(jnp.float32)
        mixed_out[j] = total.astype(jnp.bfloat16)
        across_copy(j).start()
    own_copy().wait_recv()
    for j in range(pieces):
        across_copy(j).wait_recv()
        sum_ref[j] = (
            part_ref[me, j].astype(jnp.float32)
            + own_in[j].astype(jnp.float32)
            + mixed_in[j].astype(jnp.float32)
        )
    for j in range(pieces):
        far_copy(j).wait_send()
        across_copy(j).wait_send()
    own_copy().wait_send()


def sum_branch(product):
    n_tp = lax.axis_size("tp")
    rows, width = product.shape[0] // n_tp, product.shape[1]
    pieces = max(1, rows // 16)
    depth = rows // pieces
    block = pltpu.VMEM((pieces, depth, width), jnp.bfloat16)
    many = pltpu.SemaphoreType.DMA((pieces,))
    one = pltpu.SemaphoreType.DMA
    summed = pl.pallas_call(
        functools.partial(branch_kernel, pieces),
        out_shape=jax.ShapeDtypeStruct((pieces, depth, width), jnp.float32),
        in_specs=[pl.BlockSpec(memory_space=pltpu.VMEM)],
        out_specs=pl.BlockSpec(memory_space=pltpu.VMEM),
        scratch_shapes=[block] * 4 + [many, many, one, one, many, many],
        compiler_params=pltpu.CompilerParams(collective_id=1, has_side_effects=True),
        name="sum_branch",
    )(product.reshape(n_tp, pieces, depth, width))
    return summed.reshape(rows, width)


def experts_kernel(
    n_sp,
    send_ref,
    gate_hbm,
    up_hbm,
    down_hbm,
    back_ref,
    got,
    part,
    near,
    mixed_out,
    mixed_in,
    done,
    gate,
    up,
    down,
    w_sem,
    l_sem,
    z_s,
    z_r,
    x_s,
    x_r,
    p_s,
    p_r,
    q_s,
    q_r,
    n_s,
    n_r,
    m_s,
    m_r,
    b_s,
    b_r,
):
    here = lax.axis_index("sp")
    _, across, pair, _ = tp_peers()
    weights = [
        pltpu.make_async_copy(source, target, w_sem.at[i])
        for i, (source, target) in enumerate([(gate_hbm, gate), (up_hbm, up), (down_hbm, down)])
    ]
    own_copy = pltpu.make_async_copy(send_ref.at[here], got.at[here, 0], l_sem)
    own_copy.start()
    for copy in weights:
        copy.start()
    greet(
        [{"sp": lax.rem(here + k, n_sp)} for k in range(1, n_sp)] + [{"tp": pair}, {"tp": across}]
    )

    def source_of(k):
        return lax.rem(here - k + n_sp, n_sp)

    def sp_out(k):
        there = lax.rem(here + k, n_sp)
        return push(send_ref.at[there], got.at[here, 0], z_s.at[k], z_r.at[here], {"sp": there})

    def sp_in(k):
        there = source_of(k)
        return push(send_ref.at[there], got.at[there, 0], z_s.at[k], z_r.at[there], {"sp": there})

    def spread_across(k):
        s = source_of(k)
        return push(got.at[s, 0], got.at[s, 1], x_s.at[k], x_r.at[k], {"tp": across})

    def spread_pair(k):
        s = source_of(k)
        return push(got.at[s, 0], got.at[s, 2], p_s.at[k], p_r.at[k], {"tp": pair})

    def spread_last(k):
        s = source_of(k)
        return push(got.at[s, 1], got.at[s, 3], q_s.at[k], q_r.at[k], {"tp": pair})

    def near_copy(k):
        return push(part.at[k, pl.ds(2, 2)], near.at[k], n_s.at[k], n_r.at[k], {"tp": pair})

    def mixed_copy(k):
        return push(mixed_out.at[k], mixed_in.at[k], m_s.at[k], m_r.at[k], {"tp": across})

    def back_out(k):
        s = source_of(k)
        return push(done.at[k], back_ref.at[here], b_s.at[k], b_r.at[here], {"sp": s})

    def back_in(k):
        s = lax.rem(here + k, n_sp)
        return push(done.at[k], back_ref.at[s], b_s.at[k], b_r.at[s], {"sp": s})

    def begin(k, carry):
        sp_out(k).start()
        return carry

    lax.fori_loop(1, n_sp, begin, 0)
    own_copy.wait()
    spread_across(0).start()
    spread_pair(0).start()

    def step(k, carry):
        @pl.when(k + 1 < n_sp)
        def _():
            sp_in(k + 1).wait_recv()
            spread_across(k + 1).start()
            spread_pair(k + 1).start()

        @pl.when(k < n_sp)
        def _():
            spread_across(k).wait_recv()
            spread_last(k).start()

        @pl.when(jnp.logical_and(k >= 1, k <= n_sp))
        def _():
            near_copy(k - 1).wait_recv()
            total = part[k - 1, 1].astype(jnp.float32) + near[k - 1, 1].astype(jnp.float32)
            mixed_out[k - 1] = total.astype(jnp.bfloat16)
            mixed_copy(k - 1).start()

        @pl.when(k == 0)
        def _():
            for copy in weights:
                copy.wait()

        @pl.when(k < n_sp)
        def _():
            spread_pair(k).wait_recv()
            spread_last(k).wait_recv()
            block = got[source_of(k)]
            rows = block.reshape(block.shape[0] * block.shape[1], block.shape[2])
            gate_pre = jnp.dot(rows, gate[...], preferred_element_type=jnp.float32)
            up_proj = jnp.dot(rows, up[...], preferred_element_type=jnp.float32)
            hidden = (gate_pre / (1.0 + jnp.exp(-gate_pre)) * up_proj).astype(jnp.bfloat16)
            product = jnp.dot(hidden, down[...], preferred_element_type=jnp.float32)
            part[k] = product.astype(jnp.bfloat16).reshape(block.shape)
            near_copy(k).start()

        def summed(j):
            mixed_copy(j).wait_recv()
            return (
                part[j, 0].astype(jnp.float32)
                + near[j, 0].astype(jnp.float32)
                + mixed_in[j].astype(jnp.float32)
            ).astype(jnp.bfloat16)

        @pl.when(k == 2)
        def _():
            back_ref[here] = summed(0)

        @pl.when(k > 2)
        def _():
            done[k - 2] = summed(k - 2)
            back_out(k - 2).start()

        return carry

    lax.fori_loop(0, n_sp + 2, step, 0)

    def finish(k, carry):
        spread_across(k).wait_send()
        spread_pair(k).wait_send()
        spread_last(k).wait_send()
        near_copy(k).wait_send()
        mixed_copy(k).wait_send()

        @pl.when(k >= 1)
        def _():
            sp_out(k).wait_send()
            back_out(k).wait_send()
            back_in(k).wait_recv()

        return carry

    lax.fori_loop(0, n_sp, finish, 0)


def run_experts(sending, w_gate, w_up, w_down):
    n_sp, depth, width = sending.shape
    hidden = w_gate.shape[1]
    half = jnp.bfloat16
    block = pltpu.VMEM((n_sp, depth, width), half)
    sems = pltpu.SemaphoreType.DMA((n_sp,))
    vmem = pl.BlockSpec(memory_space=pltpu.VMEM)
    hbm = pl.BlockSpec(memory_space=pl.ANY)
    flops = 6 * n_sp * 4 * depth * width * hidden
    return pl.pallas_call(
        functools.partial(experts_kernel, n_sp),
        out_shape=jax.ShapeDtypeStruct(sending.shape, half),
        in_specs=[vmem, hbm, hbm, hbm],
        out_specs=vmem,
        scratch_shapes=[
            pltpu.VMEM((n_sp, 4, depth, width), half),
            pltpu.VMEM((n_sp, 4, depth, width), half),
            pltpu.VMEM((n_sp, 2, depth, width), half),
            block,
            block,
            block,
            pltpu.VMEM((width, hidden), half),
            pltpu.VMEM((width, hidden), half),
            pltpu.VMEM((hidden, width), half),
            pltpu.SemaphoreType.DMA((3,)),
            pltpu.SemaphoreType.DMA,
        ]
        + [sems] * 14,
        compiler_params=pltpu.CompilerParams(
            collective_id=2, has_side_effects=True, vmem_limit_bytes=60 * 2**20
        ),
        cost_estimate=pl.CostEstimate(flops=flops, bytes_accessed=flops // 64, transcendentals=0),
        name="run_experts",
    )(sending, w_gate, w_up, w_down)


def body(
    residual,
    query_nope,
    query_rope,
    kv_latent,
    rope_key,
    latent_gain,
    w_key,
    w_value,
    w_out,
    post_gain,
    routes,
    route_weight,
    moe_gain,
    w_gate,
    w_up,
    w_down,
):
    tok_rows = query_nope.shape[0]
    heads_here = HEADS // lax.axis_size("tp")
    first_row = lax.axis_index("sp") * tok_rows
    positions = first_row + jnp.arange(tok_rows, dtype=jnp.int32)
    cosine_table, sine_table = tables(positions, ROPE)
    query_plain = query_nope.reshape(tok_rows, heads_here, NOPE)
    query_turned = rotate(
        query_rope.reshape(tok_rows, heads_here, ROPE).astype(jnp.float32),
        cosine_table[:, None, :],
        sine_table[:, None, :],
    ).astype(jnp.bfloat16)
    score_scale = (NOPE + ROPE) ** (-0.5)

    def update(state_now, key_plain, value_plain, key_turned):
        row_max, row_sum, running = state_now
        key_count = key_plain.shape[0]
        key_heads = key_plain.reshape(key_count, heads_here, NOPE)
        value_heads = value_plain.reshape(key_count, heads_here, VDIM)
        scores = jnp.einsum(
            "thd,shd->hts", query_plain, key_heads, preferred_element_type=jnp.float32
        )
        scores = (
            scores
            + jnp.einsum(
                "thd,sd->hts", query_turned, key_turned, preferred_element_type=jnp.float32
            )
        ) * score_scale
        key_positions = jnp.arange(key_count, dtype=jnp.int32)
        allowed = key_positions[None, :] <= positions[:, None]
        scores = jnp.where(allowed[None], scores, -1e30)
        new_max = jnp.maximum(row_max, jnp.max(scores, axis=-1))
        weights = jnp.exp(scores - new_max[..., None])
        row_sum = jnp.sum(weights, axis=-1)
        running = jnp.einsum(
            "hts,shd->htd",
            weights.astype(jnp.bfloat16),
            value_heads,
            preferred_element_type=jnp.float32,
        )
        return (new_max, row_sum, running)

    start_state = (
        jnp.full((heads_here, tok_rows), -1e30, jnp.float32),
        jnp.zeros((heads_here, tok_rows), jnp.float32),
        jnp.zeros((heads_here, tok_rows, VDIM), jnp.float32),
    )
    rank = kv_latent.shape[1]
    gathered = gather_keys(jnp.concatenate([kv_latent, rope_key], axis=1))
    pieces = (gathered[:, :rank], gathered[:, rank:])

    def take_piece(state_in):
        key_plain, value_plain, key_turned = expand(
            pieces[0], pieces[1], latent_gain, w_key, w_value
        )
        return update(state_in, key_plain, value_plain, key_turned)

    final_state = take_piece(start_state)
    attended = (final_state[2] / final_state[1][..., None]).transpose(1, 0, 2)
    attended = attended.reshape(tok_rows, heads_here * VDIM).astype(jnp.bfloat16)
    chosen = attended
    product = jnp.dot(chosen, w_out, preferred_element_type=jnp.float32)
    branch = sum_branch(product.astype(jnp.bfloat16))
    updated = (residual.astype(jnp.float32) + rms_scale(branch, post_gain)).astype(jnp.bfloat16)
    moe_in = rms_scale(updated.astype(jnp.float32), moe_gain).astype(jnp.bfloat16)
    token_count = routes.shape[0]
    experts = lax.axis_size("sp")
    capacity = max(2, 3 * token_count // experts)
    capacity = -(-capacity // 16) * 16
    onehot = (routes[:, :, None] == jnp.arange(experts, dtype=jnp.int32)[None, None, :]).astype(
        jnp.int32
    )
    flat_hits = onehot.reshape(token_count * 2, experts)
    order_in = jnp.cumsum(flat_hits, axis=0) - flat_hits
    slot_ids = jnp.sum(
        (order_in + jnp.arange(experts, dtype=jnp.int32)[None, :] * capacity) * flat_hits, axis=1
    )
    placing = slot_ids[:, None] == jnp.arange(experts * capacity, dtype=jnp.int32)[None, :]
    placing = placing.astype(jnp.bfloat16).reshape(token_count, 2, experts * capacity)
    sending = jnp.einsum("tks,td->sd", placing, moe_in, preferred_element_type=jnp.float32).astype(
        jnp.bfloat16
    )
    sending = sending.reshape(experts, capacity, sending.shape[1])
    returned = run_experts(sending, w_gate[0], w_up[0], w_down[0])
    returned = returned.reshape(experts * capacity, returned.shape[2])
    gathered_back = jnp.einsum("tks,sd->tkd", placing, returned, preferred_element_type=jnp.float32)
    weighted = jnp.sum(gathered_back * route_weight[:, :, None], axis=1)
    return (updated.astype(jnp.float32) + weighted).astype(jnp.bfloat16)


def solution(mesh):
    placed = (
        P(("grp", "sp", "tp"), None),
        P(("grp", "sp"), "tp"),
        P(("grp", "sp"), "tp"),
        P(("grp", "sp"), None),
        P(("grp", "sp"), None),
        P(),
        P(None, "tp"),
        P(None, "tp"),
        P("tp", None),
        P(),
        P(("grp", "sp", "tp"), None),
        P(("grp", "sp", "tp"), None),
        P(),
        P("sp", None, "tp"),
        P("sp", None, "tp"),
        P("sp", "tp", None),
    )
    return jax.shard_map(
        body, mesh=mesh, in_specs=placed, out_specs=P(("grp", "sp", "tp"), None), check_vma=False
    )
```
